32 devices in a mesh: grp: 2 (over y), sp: 4 (over z), tp: 4 (over x, core).
Axes of the slice: x: 2, y: 2, z: 4, core: 2. Of those that a mesh axis runs over, the one named last changes fastest.
Arguments:
- queries: bfloat16 [2048, 2048], P(('grp', 'sp'), 'tp'), parts along dimension 0, may hold values from -6 to 6
- keys: bfloat16 [2048, 512], P(('grp', 'sp'), 'tp'), parts along dimension 0, may hold values from -6 to 6
- values: bfloat16 [2048, 512], P(('grp', 'sp'), 'tp'), parts along dimension 0, may hold values from -6 to 6
- query_gain: float32 [128], replicated, may hold values from 1 to 5, as said below
- key_norm_gain: float32 [128], replicated, may hold values from 1 to 5, as said below
- out_weight: bfloat16 [2048, 2048], P('tp'), may hold values from -0.125 to 0.125
- residual: bfloat16 [2048, 2048], P(('grp', 'sp')), parts along dimension 0, may hold values from -0.59765625 to 0.59765625
- mixer_gain: float32 [2048], replicated, may hold values from 0.1 to 1.9
- gate_weight: bfloat16 [2048, 5632], P('sp', 'tp'), may hold values from -0.125 to 0.125
- up_weight: bfloat16 [2048, 5632], P('sp', 'tp'), may hold values from -0.125 to 0.125
- conv_taps: float32 [3, 5632], P(None, 'tp'), may hold values from -3.5 to 3.5
- down_weight: bfloat16 [5632, 2048], P('tp', 'sp'), may hold values from -0.078125 to 0.078125
Outputs:
- layer_out: bfloat16 [2048, 2048], P(('grp', 'sp', 'tp')), parts along dimension 0
The draws below stay inside these ranges and needn't reach their ends.
There are 2 independent parts, one for each index of `grp`. The reference program is written for one: setup_inputs(seed, part) draws one part's arguments, and reference() takes and returns one part's arrays. A program takes and returns all parts, laid end to end along the dimension named above; an argument that names none is the same for every part. Nothing has to cross between parts.
Inputs may be any that keep to these rules, and one draw needn't show every extreme that they name: `query_gain`: positive. `key_norm_gain`: positive.
All inputs are finite; a program needn't handle non-finite values.
Results may differ from the reference program's by a relative error of at most 0.024.
Values may be sent and summed in bfloat16 or wider, within the bound.
A program may use at most 128 MiB of HBM per device.

```python
import math
import jax
import jax.numpy as jnp
from jax import lax

D = 2048
FF = 5632
QUERY_HEADS = 16
KEY_VALUE_HEADS = 4
HEAD_SIZE = 128
GRID = 64
SEQUENCE_TOKENS = 1024


def grouped_keys(key):
    unit_keys = jax.random.normal(jax.random.fold_in(key, 11), (SEQUENCE_TOKENS, KEY_VALUE_HEADS * HEAD_SIZE), jnp.float32)
    return jnp.clip(unit_keys, -6.0, 6.0)


def draw_keys(key, part):
    return grouped_keys(key).astype(jnp.bfloat16)


def draw_queries(key, part):
    drawn = jnp.clip(jax.random.normal(jax.random.fold_in(key, 12), (SEQUENCE_TOKENS, QUERY_HEADS * HEAD_SIZE), jnp.float32), -6.0, 6.0)
    return drawn.astype(jnp.bfloat16)


def draw_query_gain(key, part):
    return jax.random.uniform(jax.random.fold_in(key, 21), (HEAD_SIZE,), jnp.float32, 1.0, 1.8)


def draw_key_norm_gain(key, part):
    return jax.random.uniform(jax.random.fold_in(key, 22), (HEAD_SIZE,), jnp.float32, 1.0, 1.8)


def block_levels(key, dims, shards, low, top_value):
    loudness, own = 1.0, jax.random.fold_in(key, 6)
    for axis_at, blocks in shards:
        draws = jnp.exp(jax.random.uniform(jax.random.fold_in(own, axis_at), (blocks,), jnp.float32, low / len(shards), top_value / len(shards)))
        loudness = loudness * jnp.repeat(draws, dims[axis_at] // blocks).reshape([-1 if axis == axis_at else 1 for axis in range(len(dims))])
    return loudness


def centred(key, dims, deviation, bound, pieces=(), kind=jnp.bfloat16):
    level = block_levels(key, dims, pieces, -0.22, 0.18) if pieces else 1.0
    values = jax.random.normal(key, dims, jnp.float32) * deviation * level
    return jnp.minimum(jnp.maximum(values, -bound), bound).astype(kind)


def setup_inputs(seed: int = 0, part: int = 0) -> dict:
    seeds = jax.random.split(jax.random.key(seed), 13)
    part_splits = jax.random.split(jax.random.fold_in(seeds[12], part), 13)
    return {
        "queries": draw_queries(jax.random.fold_in(jax.random.fold_in(seeds[12], part), 71), part),
        "keys": draw_keys(jax.random.fold_in(jax.random.fold_in(seeds[12], part), 71), part),
        "values": centred(part_splits[2], (SEQUENCE_TOKENS, KEY_VALUE_HEADS * HEAD_SIZE), 1.0, 6.0, ((0, 4), (1, 4))),
        "query_gain": draw_query_gain(jax.random.fold_in(seeds[12], 71), part),
        "key_norm_gain": draw_key_norm_gain(jax.random.fold_in(seeds[12], 71), part),
        "out_weight": centred(seeds[5], (QUERY_HEADS * HEAD_SIZE, D), (QUERY_HEADS * HEAD_SIZE) ** -0.5, 0.125, ((0, 4),)),
        "residual": centred(part_splits[6], (SEQUENCE_TOKENS, D), 0.1, 0.59765625, ((0, 4),)),
        "mixer_gain": jnp.clip(1.0 + 0.18 * jax.random.normal(seeds[7], (D,), jnp.float32), 0.1, 1.9),
        "gate_weight": centred(seeds[8], (D, FF), D ** -0.5, 0.125, ((0, 4), (1, 4))),
        "up_weight": centred(seeds[9], (D, FF), D ** -0.5, 0.125, ((0, 4), (1, 4))),
        "conv_taps": centred(seeds[10], (3, FF), 3 ** -0.5, 3.5, ((1, 4),), jnp.float32),
        "down_weight": centred(seeds[11], (FF, D), FF ** -0.5, 0.078125, ((0, 4), (1, 4))),
    }


norm_eps = 1e-06
rope_base = 10000.0

def angle_tables(positions, head_dim):
    quarter = head_dim // 4
    freqs = 1.0 / rope_base ** (jnp.arange(quarter, dtype=jnp.float32) * 4.0 / head_dim)
    grid_row = (positions // GRID).astype(jnp.float32)
    grid_col = (positions % GRID).astype(jnp.float32)
    by_row = grid_row[:, None] * freqs[None, :]
    by_col = grid_col[:, None] * freqs[None, :]
    angles = jnp.concatenate([by_row, by_row, by_col, by_col], axis=-1)
    return (jnp.cos(angles), jnp.sin(angles))

def apply_rotary(field, cosine_table, sine_table):
    half = field.shape[-1] // 2
    quarter = half // 2
    first = field[..., :half]
    second = field[..., half:]
    turned = jnp.concatenate([-first[..., quarter:], first[..., :quarter], -second[..., quarter:], second[..., :quarter]], axis=-1)
    return field * cosine_table[:, None, :] + turned * sine_table[:, None, :]

def per_head_norm(field, gain):
    floats = field.astype(jnp.float32)
    return floats * lax.rsqrt(lax.optimization_barrier(jnp.mean(floats * floats, axis=-1, keepdims=True)) + norm_eps) * gain

def reference(queries, keys, values, query_gain, key_norm_gain, out_weight, residual, mixer_gain, gate_weight, up_weight, conv_taps, down_weight):
    query_group = QUERY_HEADS // KEY_VALUE_HEADS
    positions = jnp.arange(SEQUENCE_TOKENS, dtype=jnp.int32)
    cosine_table, sine_table = angle_tables(positions, HEAD_SIZE)
    rotated_queries = apply_rotary(per_head_norm(queries.reshape(SEQUENCE_TOKENS, QUERY_HEADS, HEAD_SIZE), query_gain), cosine_table, sine_table).astype(jnp.bfloat16)
    rotated_keys = apply_rotary(per_head_norm(keys.reshape(SEQUENCE_TOKENS, KEY_VALUE_HEADS, HEAD_SIZE), key_norm_gain), cosine_table, sine_table).astype(jnp.bfloat16)
    key_all = rotated_keys.astype(jnp.float32)
    value_rows_full = values.reshape(SEQUENCE_TOKENS, KEY_VALUE_HEADS, HEAD_SIZE).astype(jnp.float32)
    block_slice = math.gcd(SEQUENCE_TOKENS, 512)
    query_block_list = rotated_queries.reshape(SEQUENCE_TOKENS // block_slice, block_slice, KEY_VALUE_HEADS, query_group, HEAD_SIZE)
    scale = HEAD_SIZE ** (-0.5)

    def one_block(query_block):
        scores = jnp.einsum('qhgd,khd->hgqk', query_block.astype(jnp.float32), key_all) * scale
        expo = jnp.exp(scores - lax.optimization_barrier(jnp.max(scores, axis=-1, keepdims=True)))
        totals = lax.optimization_barrier(jnp.sum(expo, axis=-1))
        weights = lax.optimization_barrier(expo.astype(jnp.bfloat16)).astype(jnp.float32)
        summed = jnp.einsum('hgqk,khd->qhgd', weights, value_rows_full)
        return (summed / jnp.transpose(totals, (2, 0, 1))[..., None]).astype(jnp.bfloat16)
    heads = lax.map(one_block, query_block_list).reshape(SEQUENCE_TOKENS, QUERY_HEADS * HEAD_SIZE)
    mixed = residual.astype(jnp.float32) + jnp.dot(heads, out_weight, preferred_element_type=jnp.float32)
    normed = per_head_norm(mixed, mixer_gain).astype(jnp.bfloat16)
    gate = jnp.dot(normed, gate_weight, preferred_element_type=jnp.float32).astype(jnp.bfloat16)
    up_val = jnp.dot(normed, up_weight, preferred_element_type=jnp.float32).astype(jnp.bfloat16)
    padded = jnp.pad(gate.astype(jnp.float32), ((1, 1), (0, 0)))
    conv = conv_taps[0] * padded[:-2] + conv_taps[1] * padded[1:-1] + conv_taps[2] * padded[2:]
    hidden = (jax.nn.silu(conv) * up_val.astype(jnp.float32)).astype(jnp.bfloat16)
    layer_out = mixed + jnp.dot(hidden, down_weight, preferred_element_type=jnp.float32)
    return layer_out.astype(jnp.bfloat16)
```

```python
import functools
import math

import jax
import jax.numpy as jnp
from jax import lax
from jax.experimental import pallas as pl
from jax.experimental.pallas import tpu as pltpu
from jax.sharding import PartitionSpec as P

GRID = 64


norm_eps = 1e-06
rope_base = 10000.0


def padded_2(block, sides, width):
    for axis, dim in sides:
        count = lax.axis_size(axis)
        forward = [(i, i + 1) for i in range(count - 1)]
        backward = [(target, source) for source, target in forward]
        low = lax.ppermute(
            lax.slice_in_dim(block, block.shape[dim] - width, None, axis=dim), axis, forward
        )
        high = lax.ppermute(lax.slice_in_dim(block, 0, width, axis=dim), axis, backward)
        block = jnp.concatenate([low, block, high], axis=dim)
    return block


def angle_tables(positions, head_dim):
    quarter = head_dim // 4
    freqs = 1.0 / rope_base ** (jnp.arange(quarter, dtype=jnp.float32) * 4.0 / head_dim)
    grid_row = (positions // GRID).astype(jnp.float32)
    grid_col = (positions % GRID).astype(jnp.float32)
    by_row = grid_row[:, None] * freqs[None, :]
    by_col = grid_col[:, None] * freqs[None, :]
    angles = jnp.concatenate([by_row, by_row, by_col, by_col], axis=-1)
    return (jnp.cos(angles), jnp.sin(angles))


def apply_rotary(field, cosine_table, sine_table):
    half = field.shape[-1] // 2
    quarter = half // 2
    first = field[..., :half]
    second = field[..., half:]
    turned = jnp.concatenate(
        [
            -first[..., quarter:],
            first[..., :quarter],
            -second[..., quarter:],
            second[..., :quarter],
        ],
        axis=-1,
    )
    return field * cosine_table[:, None, :] + turned * sine_table[:, None, :]


def per_head_norm(field, gain):
    floats = field.astype(jnp.float32)
    return floats * lax.rsqrt(jnp.mean(floats * floats, axis=-1, keepdims=True) + norm_eps) * gain


def local(
    queries,
    keys,
    values,
    query_gain,
    key_norm_gain,
    out_weight,
    residual,
    mixer_gain,
    gate_weight,
    up_weight,
    conv_taps,
    down_weight,
):
    tok_rows = queries.shape[0]
    head_dim = query_gain.shape[0]
    heads_here = queries.shape[1] // head_dim
    kv_here = keys.shape[1] // head_dim
    query_group = heads_here // kv_here
    part_rows = tok_rows // lax.axis_size("tp")
    positions = lax.axis_index("sp") * tok_rows + jnp.arange(tok_rows, dtype=jnp.int32)
    cosine_table, sine_table = angle_tables(positions, head_dim)
    rotated_queries = apply_rotary(
        per_head_norm(queries.reshape(tok_rows, heads_here, head_dim), query_gain),
        cosine_table,
        sine_table,
    ).astype(jnp.bfloat16)
    rotated_keys = apply_rotary(
        per_head_norm(keys.reshape(tok_rows, kv_here, head_dim), key_norm_gain),
        cosine_table,
        sine_table,
    ).astype(jnp.bfloat16)
    key_flat = rotated_keys.reshape(tok_rows, kv_here * head_dim)
    query_mat = jnp.transpose(
        rotated_queries.reshape(tok_rows, kv_here, query_group, head_dim), (1, 2, 0, 3)
    )
    query_mat = query_mat.reshape(kv_here, query_group * tok_rows, head_dim)
    scale = head_dim ** (-0.5)
    start_state = (
        jnp.full((kv_here, query_group * tok_rows), -jnp.inf, jnp.float32),
        jnp.zeros((kv_here, query_group * tok_rows), jnp.float32),
        jnp.zeros((kv_here, query_group * tok_rows, head_dim), jnp.float32),
    )
    key_piece = lax.all_gather(key_flat, "sp", axis=0, tiled=True)
    value_piece = lax.all_gather(values, "sp", axis=0, tiled=True)
    piece_rows = key_piece.shape[0]
    block_slice = math.gcd(piece_rows, 512)
    key_blocks = key_piece.reshape(piece_rows // block_slice, block_slice, kv_here, head_dim)
    value_blocks = value_piece.reshape(piece_rows // block_slice, block_slice, kv_here, head_dim)

    def one_block(state, block_pair):
        running, totals, accum = state
        key_block, value_block = block_pair
        scores = (
            jnp.einsum("hqd,khd->hqk", query_mat, key_block, preferred_element_type=jnp.float32)
            * scale
        )
        new_max = jnp.maximum(running, jnp.max(scores, axis=-1))
        factor = jnp.exp(running - new_max)
        expo = jnp.exp(scores - new_max[..., None])
        totals = totals * factor + jnp.sum(expo, axis=-1)
        accum = accum * factor[..., None] + jnp.einsum(
            "hqk,khd->hqd",
            expo.astype(jnp.bfloat16),
            value_block,
            preferred_element_type=jnp.float32,
        )
        return ((new_max, totals, accum), None)

    result, unused = lax.scan(one_block, start_state, (key_blocks, value_blocks))
    running, totals, accum = result
    heads = (accum / totals[..., None]).astype(jnp.bfloat16)
    heads = jnp.transpose(heads.reshape(kv_here, query_group, tok_rows, head_dim), (2, 0, 1, 3))
    heads = heads.reshape(tok_rows, heads_here * head_dim)
    own_start = lax.axis_index("tp") * part_rows
    full_proj = lax.psum(
        jnp.dot(heads, out_weight, preferred_element_type=jnp.float32).astype(jnp.bfloat16), "tp"
    ).astype(jnp.float32)
    mixed = residual.astype(jnp.float32) + full_proj
    normed = per_head_norm(mixed, mixer_gain).astype(jnp.bfloat16)
    mixed_keep = lax.dynamic_slice_in_dim(mixed, own_start, part_rows, 0)
    gate_acc = jnp.dot(
        normed,
        lax.all_gather(gate_weight, "sp", axis=0, tiled=True),
        preferred_element_type=jnp.float32,
    )
    up_acc = jnp.dot(
        normed,
        lax.all_gather(up_weight, "sp", axis=0, tiled=True),
        preferred_element_type=jnp.float32,
    )
    gate = gate_acc.astype(jnp.bfloat16)
    up_val = up_acc.astype(jnp.bfloat16)
    padded = padded_2(gate, (("sp", 0),), 1).astype(jnp.float32)
    conv = conv_taps[0] * padded[:-2] + conv_taps[1] * padded[1:-1] + conv_taps[2] * padded[2:]
    hidden = (jax.nn.silu(conv) * up_val.astype(jnp.float32)).astype(jnp.bfloat16)
    down_full = lax.all_gather(down_weight, "sp", axis=1, tiled=True)
    mixer_out = lax.psum_scatter(
        jnp.dot(hidden, down_full, preferred_element_type=jnp.float32).astype(jnp.bfloat16),
        "tp",
        scatter_dimension=0,
        tiled=True,
    ).astype(jnp.float32)
    return (mixed_keep + mixer_out).astype(jnp.bfloat16)


MESH_ID = pl.DeviceIdType.MESH
LANES = 128


def fused_kernel(
    n, width, q_ref, k_ref, v_ref, qg_ref, kg_ref, cos_ref, sa_ref, sb_ref, mg_ref, taps_ref,
    ow_hbm, res_hbm, gw_hbm, uw_hbm, dw_hbm, out_ref,
    kv, heads, ow, res, pbuf, rc, xs, rx, mixed, ng, wg, wu, wd, gate, up, ps, prc, pxs, prx,
    pzs, pzr, lsem, kv_s, kv_r, w_s, w_r, y_s, y_r, a_s, a_r, z_s, z_r, x_s, x_r, c_s, c_r,
    pc_s, pc_r, px_s, px_r, pz_s, pz_r,
):
    f32, bf16 = jnp.float32, jnp.bfloat16
    s = lax.axis_index("sp")
    t = lax.axis_index("tp")
    g = lax.axis_index("grp")
    c = lax.rem(t, 2)
    x = t // 2
    core_id = {"tp": 2 * x + 1 - c}
    x_id = {"tp": lax.rem(t + 2, 4)}
    y_id = {"grp": 1 - g}
    rows, hd = k_ref.shape
    hq = q_ref.shape[1] // hd
    depth = gw_hbm.shape[0]
    half = depth // 2
    hidden_here = gw_hbm.shape[1]
    part = rows // 4
    sends = []

    def sp_of(d):
        return lax.rem(s + d, n)

    def col_start(j):
        return pl.multiple_of(j * width - (j // (n - 1)) * (n * width - hidden_here), LANES)

    def send(src, dst, ssem, rsem, dev):
        copy = pltpu.make_async_remote_copy(
            src_ref=src, dst_ref=dst, send_sem=ssem, recv_sem=rsem, device_id=dev,
            device_id_type=MESH_ID,
        )
        copy.start()
        sends.append(copy)
        return copy

    barrier = pltpu.get_barrier_semaphore()
    peers = [{"sp": sp_of(d)} for d in range(1, n)] + [core_id, x_id, y_id]
    for dev in peers:
        pl.semaphore_signal(barrier, inc=1, device_id=dev, device_id_type=MESH_ID)

    mine = col_start(s)
    block = pl.ds(pl.multiple_of(s * depth, depth), depth)
    local = [
        pltpu.make_async_copy(ow_hbm, ow, lsem.at[0]),
        pltpu.make_async_copy(
            res_hbm.at[pl.ds(pl.multiple_of(t * part, part), part)], res, lsem.at[1]
        ),
        pltpu.make_async_copy(gw_hbm.at[:, pl.ds(mine, width)], wg.at[block], lsem.at[2]),
        pltpu.make_async_copy(uw_hbm.at[:, pl.ds(mine, width)], wu.at[block], lsem.at[3]),
        pltpu.make_async_copy(dw_hbm.at[pl.ds(mine, width)], wd.at[s], lsem.at[4]),
    ]
    for copy in local:
        copy.start()

    cos, sa, sb = cos_ref[...], sa_ref[...], sb_ref[...]

    def rotated(field, gain):
        y = field.astype(f32)
        y = y * lax.rsqrt(jnp.mean(y * y, axis=-1, keepdims=True) + norm_eps) * gain
        return (
            y * cos + pltpu.roll(y, hd // 4, 1) * sa + pltpu.roll(y, hd - hd // 4, 1) * sb
        ).astype(bf16)

    kv[s, :, :hd] = rotated(k_ref[...], kg_ref[...])
    kv[s, :, hd:] = v_ref[...]
    pl.semaphore_wait(barrier, len(peers))
    kv_copies = [
        send(kv.at[s], kv.at[s], kv_s.at[d], kv_r.at[d], {"sp": sp_of(d)}) for d in range(1, n)
    ]

    def wrows(base):
        return pl.ds(pl.multiple_of(base * depth + g * half, half), half)

    whalf = pl.ds(pl.multiple_of(g * half, half), half)
    hw = width // 2
    dhalf = pl.ds(pl.multiple_of(g * hw, hw), hw)
    w_copies = []
    for d in range(1, n):
        j = sp_of(d)
        for i, (hbm, dst) in enumerate(((gw_hbm, wg), (uw_hbm, wu))):
            w_copies.append(
                send(hbm.at[whalf, pl.ds(col_start(j), width)], dst.at[wrows(s)],
                     w_s.at[i, d], w_r.at[i, d], {"sp": j})
            )

    def query(h):
        return rotated(q_ref[:, h * hd : (h + 1) * hd], qg_ref[...])

    queries = [query(h) for h in range(hq)]
    for copy in kv_copies:
        copy.wait_recv()
    key_all = kv[:, :, :hd].reshape(n * rows, hd)
    value_all = kv[:, :, hd:].reshape(n * rows, hd)
    scale = hd ** (-0.5)
    for h in range(hq):
        scores = lax.dot_general(
            queries[h], key_all, (((1,), (1,)), ((), ())), preferred_element_type=f32
        ) * scale
        expo = jnp.exp(scores - jnp.max(scores, axis=-1, keepdims=True))
        totals = jnp.sum(expo, axis=-1, keepdims=True)
        mix = jnp.dot(expo.astype(bf16), value_all, preferred_element_type=f32) / totals
        heads[:, h * hd : (h + 1) * hd] = mix.astype(bf16)
    local[0].wait()
    dim = ow.shape[1]
    pbuf[...] = (
        jnp.dot(heads[...], ow[...], preferred_element_type=f32).astype(bf16)
        .reshape(4, part, dim)
    )
    a_copies = [
        send(pbuf.at[2 * e + 1 - c], rc.at[e], a_s.at[e], a_r.at[e], core_id) for e in range(2)
    ]
    for copy in a_copies:
        copy.wait_recv()
    xs[...] = (
        pbuf[2 * (1 - x) + c].astype(f32) + rc[1 - x].astype(f32)
    ).astype(bf16)
    ax = send(xs, rx, a_s.at[2], a_r.at[2], x_id)
    local[1].wait()
    ax.wait_recv()
    total = pbuf[t].astype(f32) + rc[x].astype(f32) + rx[...].astype(f32)
    total = total + res[...].astype(f32)
    mixed[...] = total
    ng[s, t] = (
        total * lax.rsqrt(jnp.mean(total * total, axis=-1, keepdims=True) + norm_eps)
        * mg_ref[...]
    ).astype(bf16)

    own = ng.at[s, t]
    z_copies = [None] + [
        send(own, own, z_s.at[d], z_r.at[d], {"sp": sp_of(d)}) for d in range(1, n)
    ]
    x_copies, c_copies = [], []

    def relay(d):
        piece = ng.at[sp_of(n - d), t]
        x_copies.append(send(piece, piece, x_s.at[d], x_r.at[d], x_id))
        c_copies.append(send(piece, piece, c_s.at[0, d], c_r.at[0, d], core_id))

    relay(0)
    d_copies = []
    for d in range(1, n):
        j = sp_of(d)
        rows_j = pl.ds(pl.multiple_of(col_start(j) + g * hw, LANES // 2), hw)
        d_copies.append(
            send(dw_hbm.at[rows_j], wd.at[s, dhalf], w_s.at[2, d], w_r.at[2, d], {"sp": j})
        )
    y_copies = []
    k = 0
    for d in range(1, n):
        for i, dst in enumerate((wg, wu)):
            w_copies[k].wait_recv()
            k += 1
            piece = dst.at[wrows(sp_of(n - d))]
            y_copies.append(send(piece, piece, y_s.at[i, d], y_r.at[i, d], y_id))

    gate[0:8] = jnp.zeros((8, width), f32)
    gate[n * rows + 8 : n * rows + 16] = jnp.zeros((8, width), f32)
    for d in range(n):
        if d + 1 < n:
            z_copies[d + 1].wait_recv()
            relay(d + 1)
        x_copies[d].wait_recv()
        src = sp_of(n - d)
        piece = ng.at[src, lax.rem(t + 2, 4)]
        fwd = send(piece, piece, c_s.at[1, d], c_r.at[1, d], core_id)
        if d == 0:
            local[2].wait()
            local[3].wait()
            for copy in y_copies:
                copy.wait_recv()
        c_copies[d].wait_recv()
        fwd.wait_recv()
        tokens = ng[src].reshape(rows, dim)
        at = pl.ds(pl.multiple_of(src * rows + 8, 8), rows)
        gate[at] = jnp.dot(tokens, wg[...], preferred_element_type=f32).astype(bf16).astype(f32)
        up[src] = jnp.dot(tokens, wu[...], preferred_element_type=f32).astype(bf16)
    yd_copies = []
    for d in range(1, n):
        d_copies[d - 1].wait_recv()
        piece = wd.at[sp_of(n - d), dhalf]
        yd_copies.append(send(piece, piece, y_s.at[2, d], y_r.at[2, d], y_id))
    column = mine + lax.broadcasted_iota(jnp.int32, (rows, width), 1)
    keep = column >= s * width

    def stage_hidden(i):
        dst = sp_of(1 + i)
        window = gate[pl.ds(pl.multiple_of(dst * rows, 8), rows + 16)]
        taps = taps_ref[...]
        conv = (
            taps[0:1] * window[7 : 7 + rows]
            + taps[1:2] * window[8 : 8 + rows]
            + taps[2:3] * window[9 : 9 + rows]
        )
        hid = jax.nn.silu(conv) * up[dst].astype(f32)
        return jnp.where(keep, hid, 0.0).astype(bf16)

    pcs, pxc, pzc = {}, {}, {}

    def stage_a(i):
        hid = stage_hidden(i)
        if i == 0:
            local[4].wait()
            for copy in yd_copies:
                copy.wait_recv()
        for b in range(n):
            ps[i, :, :, b * depth : (b + 1) * depth] = (
                jnp.dot(hid, wd[b], preferred_element_type=f32).astype(bf16)
                .reshape(4, part, depth)
            )
        pcs[i] = [
            send(ps.at[i, 2 * e + 1 - c], prc.at[i, e], pc_s.at[i, e], pc_r.at[i, e], core_id)
            for e in range(2)
        ]

    def stage_b(i):
        for copy in pcs[i]:
            copy.wait_recv()
        pxs[i] = (
            ps[i, 2 * (1 - x) + c].astype(f32) + prc[i, 1 - x].astype(f32)
        ).astype(bf16)
        pxc[i] = send(pxs.at[i], prx.at[i], px_s.at[i], px_r.at[i], x_id)

    def stage_c(i):
        pxc[i].wait_recv()
        total = ps[i, t].astype(f32) + prc[i, x].astype(f32) + prx[i].astype(f32)
        if i == n - 1:
            mixed[...] += total
        else:
            pzs[i] = total.astype(bf16)
            pzc[i] = send(pzs.at[i], pzr.at[i], pz_s.at[i], pz_r.at[i], {"sp": sp_of(1 + i)})

    for i in range(n + 2):
        if i < n:
            stage_a(i)
        if 0 <= i - 1 < n:
            stage_b(i - 1)
        if 0 <= i - 2 < n:
            stage_c(i - 2)
    final = mixed[...]
    for i in range(n - 1):
        pzc[i].wait_recv()
        final = final + pzr[i].astype(f32)
    out_ref[...] = final.astype(bf16)
    for copy in sends:
        copy.wait_send()


def fused(n, width, queries, keys, values, query_gain, key_norm_gain, out_weight, residual,
          mixer_gain, gate_weight, up_weight, conv_taps, down_weight):
    rows, hd = keys.shape
    dim = residual.shape[1]
    part = rows // 4
    bf16, f32 = jnp.bfloat16, jnp.float32
    s = lax.axis_index("sp")
    positions = s * rows + jnp.arange(rows, dtype=jnp.int32)
    cos, sin = angle_tables(positions, hd)
    odd = (jnp.arange(hd) // (hd // 4)) % 2 == 1
    sa = jnp.where(odd, sin, 0.0)
    sb = jnp.where(odd, 0.0, -sin)
    start = jnp.minimum(s * width, conv_taps.shape[1] - width)
    taps = lax.dynamic_slice_in_dim(conv_taps, start, width, 1)
    vm = pl.BlockSpec(memory_space=pltpu.VMEM)
    hbm = pl.BlockSpec(memory_space=pl.ANY)
    dma = pltpu.SemaphoreType.DMA
    V = pltpu.VMEM
    scratch = [
        V((n, rows, 2 * hd), bf16), V((rows, queries.shape[1]), bf16),
        V(out_weight.shape, bf16), V((part, dim), bf16), V((4, part, dim), bf16),
        V((2, part, dim), bf16), V((part, dim), bf16), V((part, dim), bf16), V((part, dim), f32),
        V((n, 4, part, dim), bf16), V((dim, width), bf16), V((dim, width), bf16),
        V((n, width, dim // n), bf16), V((n * rows + 16, width), f32), V((n, rows, width), bf16),
        V((n, 4, part, dim), bf16), V((n, 2, part, dim), bf16), V((n, part, dim), bf16),
        V((n, part, dim), bf16), V((n - 1, part, dim), bf16), V((n - 1, part, dim), bf16),
        dma((5,)), dma((n,)), dma((n,)), dma((3, n)), dma((3, n)), dma((3, n)), dma((3, n)),
        dma((3,)), dma((3,)), dma((n,)), dma((n,)), dma((n,)), dma((n,)), dma((2, n)),
        dma((2, n)), dma((n, 2)), dma((n, 2)), dma((n,)), dma((n,)), dma((n,)), dma((n,)),
    ]
    return pl.pallas_call(
        functools.partial(fused_kernel, n, width),
        out_shape=jax.ShapeDtypeStruct((part, dim), bf16),
        in_specs=[vm] * 10 + [hbm] * 5,
        out_specs=vm,
        scratch_shapes=scratch,
        compiler_params=pltpu.CompilerParams(
            collective_id=0, has_side_effects=True, vmem_limit_bytes=60 * 1024 * 1024
        ),
    )(queries, keys, values, query_gain[None], key_norm_gain[None], cos, sa, sb,
      mixer_gain[None], taps, out_weight, residual, gate_weight, up_weight, down_weight)


def block_width(n, hidden_here):
    return -(-hidden_here // (n * LANES)) * LANES


def dispatch(*args):
    queries, keys, gate_weight = args[0], args[1], args[8]
    n = lax.axis_size("sp")
    hidden_here = gate_weight.shape[1]
    width = block_width(n, hidden_here)
    fits = (n - 1) * width < hidden_here and n * keys.shape[0] <= 2048
    if (
        n > 1 and fits and lax.axis_size("tp") == 4 and lax.axis_size("grp") == 2
        and keys.shape[1] == args[3].shape[0] and keys.shape[0] % 64 == 0
        and hidden_here % LANES == 0
    ):
        return fused(n, width, *args)
    return local(*args)


def solution(mesh):
    in_specs = (
        P(("grp", "sp"), "tp"),
        P(("grp", "sp"), "tp"),
        P(("grp", "sp"), "tp"),
        P(),
        P(),
        P("tp", None),
        P(("grp", "sp"), None),
        P(),
        P("sp", "tp"),
        P("sp", "tp"),
        P(None, "tp"),
        P("tp", "sp"),
    )
    out_specs = P(("grp", "sp", "tp"), None)
    return jax.shard_map(dispatch, mesh=mesh, in_specs=in_specs, out_specs=out_specs, check_vma=False)
```

```python
import functools
import math

import jax
import jax.numpy as jnp
from jax import lax
from jax.experimental import pallas as pl
from jax.experimental.pallas import tpu as pltpu
from jax.sharding import PartitionSpec as P

GRID = 64


norm_eps = 1e-06
rope_base = 10000.0


def padded_2(block, sides, width):
    for axis, dim in sides:
        count = lax.axis_size(axis)
        forward = [(i, i + 1) for i in range(count - 1)]
        backward = [(target, source) for source, target in forward]
        low = lax.ppermute(
            lax.slice_in_dim(block, block.shape[dim] - width, None, axis=dim), axis, forward
        )
        high = lax.ppermute(lax.slice_in_dim(block, 0, width, axis=dim), axis, backward)
        block = jnp.concatenate([low, block, high], axis=dim)
    return block


def angle_tables(positions, head_dim):
    quarter = head_dim // 4
    freqs = 1.0 / rope_base ** (jnp.arange(quarter, dtype=jnp.float32) * 4.0 / head_dim)
    grid_row = (positions // GRID).astype(jnp.float32)
    grid_col = (positions % GRID).astype(jnp.float32)
    by_row = grid_row[:, None] * freqs[None, :]
    by_col = grid_col[:, None] * freqs[None, :]
    angles = jnp.concatenate([by_row, by_row, by_col, by_col], axis=-1)
    return (jnp.cos(angles), jnp.sin(angles))


def apply_rotary(field, cosine_table, sine_table):
    half = field.shape[-1] // 2
    quarter = half // 2
    first = field[..., :half]
    second = field[..., half:]
    turned = jnp.concatenate(
        [
            -first[..., quarter:],
            first[..., :quarter],
            -second[..., quarter:],
            second[..., :quarter],
        ],
        axis=-1,
    )
    return field * cosine_table[:, None, :] + turned * sine_table[:, None, :]


def per_head_norm(field, gain):
    floats = field.astype(jnp.float32)
    return floats * lax.rsqrt(jnp.mean(floats * floats, axis=-1, keepdims=True) + norm_eps) * gain


def local(
    queries,
    keys,
    values,
    query_gain,
    key_norm_gain,
    out_weight,
    residual,
    mixer_gain,
    gate_weight,
    up_weight,
    conv_taps,
    down_weight,
):
    tok_rows = queries.shape[0]
    head_dim = query_gain.shape[0]
    heads_here = queries.shape[1] // head_dim
    kv_here = keys.shape[1] // head_dim
    query_group = heads_here // kv_here
    part_rows = tok_rows // lax.axis_size("tp")
    positions = lax.axis_index("sp") * tok_rows + jnp.arange(tok_rows, dtype=jnp.int32)
    cosine_table, sine_table = angle_tables(positions, head_dim)
    rotated_queries = apply_rotary(
        per_head_norm(queries.reshape(tok_rows, heads_here, head_dim), query_gain),
        cosine_table,
        sine_table,
    ).astype(jnp.bfloat16)
    rotated_keys = apply_rotary(
        per_head_norm(keys.reshape(tok_rows, kv_here, head_dim), key_norm_gain),
        cosine_table,
        sine_table,
    ).astype(jnp.bfloat16)
    key_flat = rotated_keys.reshape(tok_rows, kv_here * head_dim)
    query_mat = jnp.transpose(
        rotated_queries.reshape(tok_rows, kv_here, query_group, head_dim), (1, 2, 0, 3)
    )
    query_mat = query_mat.reshape(kv_here, query_group * tok_rows, head_dim)
    scale = head_dim ** (-0.5)
    start_state = (
        jnp.full((kv_here, query_group * tok_rows), -jnp.inf, jnp.float32),
        jnp.zeros((kv_here, query_group * tok_rows), jnp.float32),
        jnp.zeros((kv_here, query_group * tok_rows, head_dim), jnp.float32),
    )
    key_piece = lax.all_gather(key_flat, "sp", axis=0, tiled=True)
    value_piece = lax.all_gather(values, "sp", axis=0, tiled=True)
    piece_rows = key_piece.shape[0]
    block_slice = math.gcd(piece_rows, 512)
    key_blocks = key_piece.reshape(piece_rows // block_slice, block_slice, kv_here, head_dim)
    value_blocks = value_piece.reshape(piece_rows // block_slice, block_slice, kv_here, head_dim)

    def one_block(state, block_pair):
        running, totals, accum = state
        key_block, value_block = block_pair
        scores = (
            jnp.einsum("hqd,khd->hqk", query_mat, key_block, preferred_element_type=jnp.float32)
            * scale
        )
        new_max = jnp.maximum(running, jnp.max(scores, axis=-1))
        factor = jnp.exp(running - new_max)
        expo = jnp.exp(scores - new_max[..., None])
        totals = totals * factor + jnp.sum(expo, axis=-1)
        accum = accum * factor[..., None] + jnp.einsum(
            "hqk,khd->hqd",
            expo.astype(jnp.bfloat16),
            value_block,
            preferred_element_type=jnp.float32,
        )
        return ((new_max, totals, accum), None)

    result, unused = lax.scan(one_block, start_state, (key_blocks, value_blocks))
    running, totals, accum = result
    heads = (accum / totals[..., None]).astype(jnp.bfloat16)
    heads = jnp.transpose(heads.reshape(kv_here, query_group, tok_rows, head_dim), (2, 0, 1, 3))
    heads = heads.reshape(tok_rows, heads_here * head_dim)
    own_start = lax.axis_index("tp") * part_rows
    full_proj = lax.psum(
        jnp.dot(heads, out_weight, preferred_element_type=jnp.float32).astype(jnp.bfloat16), "tp"
    ).astype(jnp.float32)
    mixed = residual.astype(jnp.float32) + full_proj
    normed = per_head_norm(mixed, mixer_gain).astype(jnp.bfloat16)
    mixed_keep = lax.dynamic_slice_in_dim(mixed, own_start, part_rows, 0)
    gate_acc = jnp.dot(
        normed,
        lax.all_gather(gate_weight, "sp", axis=0, tiled=True),
        preferred_element_type=jnp.float32,
    )
    up_acc = jnp.dot(
        normed,
        lax.all_gather(up_weight, "sp", axis=0, tiled=True),
        preferred_element_type=jnp.float32,
    )
    gate = gate_acc.astype(jnp.bfloat16)
    up_val = up_acc.astype(jnp.bfloat16)
    padded = padded_2(gate, (("sp", 0),), 1).astype(jnp.float32)
    conv = conv_taps[0] * padded[:-2] + conv_taps[1] * padded[1:-1] + conv_taps[2] * padded[2:]
    hidden = (jax.nn.silu(conv) * up_val.astype(jnp.float32)).astype(jnp.bfloat16)
    down_full = lax.all_gather(down_weight, "sp", axis=1, tiled=True)
    mixer_out = lax.psum_scatter(
        jnp.dot(hidden, down_full, preferred_element_type=jnp.float32).astype(jnp.bfloat16),
        "tp",
        scatter_dimension=0,
        tiled=True,
    ).astype(jnp.float32)
    return (mixed_keep + mixer_out).astype(jnp.bfloat16)


MESH_ID = pl.DeviceIdType.MESH
LANES = 128


def fused_kernel(
    n, width, q_ref, k_ref, v_ref, qg_ref, kg_ref, cos_ref, sa_ref, sb_ref, mg_ref,
    ow_hbm, res_hbm, gw_hbm, uw_hbm, dw_hbm, taps_hbm, out_ref,
    kv, heads, ow, res, pbuf, rc, xs, rx, mixed, ng, wg, wu, wd, taps_ref, gate, up, hid, ps, prc, pxs, prx,
    pzs, pzr, lsem, kv_s, kv_r, w_s, w_r, y_s, y_r, a_s, a_r, z_s, z_r, x_s, x_r, c_s, c_r,
    pc_s, pc_r, px_s, px_r, pz_s, pz_r,
):
    f32, bf16 = jnp.float32, jnp.bfloat16
    s = lax.axis_index("sp")
    t = lax.axis_index("tp")
    g = lax.axis_index("grp")
    c = lax.rem(t, 2)
    x = t // 2
    core_id = {"tp": 2 * x + 1 - c}
    x_id = {"tp": lax.rem(t + 2, 4)}
    y_id = {"grp": 1 - g}
    rows, hd = k_ref.shape
    hq = q_ref.shape[1] // hd
    depth = gw_hbm.shape[0]
    half = depth // 2
    hidden_here = gw_hbm.shape[1]
    part = rows // 4
    cols = dw_hbm.shape[1]
    sends = []

    def sp_of(d):
        return lax.rem(s + d, n)

    def col_start(j):
        return pl.multiple_of(j * width - (j // (n - 1)) * (n * width - hidden_here), LANES)

    def send(src, dst, ssem, rsem, dev):
        copy = pltpu.make_async_remote_copy(
            src_ref=src, dst_ref=dst, send_sem=ssem, recv_sem=rsem, device_id=dev,
            device_id_type=MESH_ID,
        )
        copy.start()
        sends.append(copy)
        return copy

    barrier = pltpu.get_barrier_semaphore()
    peers = [{"sp": sp_of(d)} for d in range(1, n)] + [core_id, x_id, y_id]
    for dev in peers:
        pl.semaphore_signal(barrier, inc=1, device_id=dev, device_id_type=MESH_ID)

    mine = col_start(s)
    block = pl.ds(pl.multiple_of(s * depth, depth), depth)
    local = [
        pltpu.make_async_copy(ow_hbm, ow, lsem.at[0]),
        pltpu.make_async_copy(
            res_hbm.at[pl.ds(pl.multiple_of(t * part, part), part)], res, lsem.at[1]
        ),
        pltpu.make_async_copy(gw_hbm.at[:, pl.ds(mine, width)], wg.at[block], lsem.at[2]),
        pltpu.make_async_copy(uw_hbm.at[:, pl.ds(mine, width)], wu.at[block], lsem.at[3]),
        pltpu.make_async_copy(dw_hbm.at[pl.ds(mine, width)], wd.at[s], lsem.at[4]),
        pltpu.make_async_copy(taps_hbm.at[:, pl.ds(mine, width)], taps_ref, lsem.at[5]),
    ]
    for copy in local:
        copy.start()

    cos, sa, sb = cos_ref[...], sa_ref[...], sb_ref[...]

    def rotated(field, gain):
        y = field.astype(f32)
        y = y * lax.rsqrt(jnp.mean(y * y, axis=-1, keepdims=True) + norm_eps) * gain
        return (
            y * cos + pltpu.roll(y, hd // 4, 1) * sa + pltpu.roll(y, hd - hd // 4, 1) * sb
        ).astype(bf16)

    kv[s, :, :hd] = rotated(k_ref[...], kg_ref[...])
    kv[s, :, hd:] = v_ref[...]
    pl.semaphore_wait(barrier, len(peers))
    kv_copies = [
        send(kv.at[s], kv.at[s], kv_s.at[d], kv_r.at[d], {"sp": sp_of(d)}) for d in range(1, n)
    ]

    def wrows(base):
        return pl.ds(pl.multiple_of(base * depth + g * half, half), half)

    whalf = pl.ds(pl.multiple_of(g * half, half), half)
    hw = width // 2
    dhalf = pl.ds(pl.multiple_of(g * hw, hw), hw)
    w_copies = []
    for d in range(1, n):
        j = sp_of(d)
        for i, (hbm, dst) in enumerate(((gw_hbm, wg), (uw_hbm, wu))):
            w_copies.append(
                send(hbm.at[whalf, pl.ds(col_start(j), width)], dst.at[wrows(s)],
                     w_s.at[i, d], w_r.at[i, d], {"sp": j})
            )

    def query(h):
        return rotated(q_ref[:, h * hd : (h + 1) * hd], qg_ref[...])

    queries = [query(h) for h in range(hq)]
    for copy in kv_copies:
        copy.wait_recv()
    key_all = kv[:, :, :hd].reshape(n * rows, hd)
    value_all = kv[:, :, hd:].reshape(n * rows, hd)
    scale = hd ** (-0.5)
    for h in range(hq):
        scores = lax.dot_general(
            queries[h], key_all, (((1,), (1,)), ((), ())), preferred_element_type=f32
        ) * scale
        expo = jnp.exp(scores - jnp.max(scores, axis=-1, keepdims=True))
        totals = jnp.sum(expo, axis=-1, keepdims=True)
        mix = jnp.dot(expo.astype(bf16), value_all, preferred_element_type=f32) / totals
        heads[:, h * hd : (h + 1) * hd] = mix.astype(bf16)
    local[0].wait()
    dim = ow.shape[1]
    pbuf[...] = (
        jnp.dot(heads[...], ow[...], preferred_element_type=f32).astype(bf16)
        .reshape(4, part, dim)
    )
    a_copies = [
        send(pbuf.at[2 * e + 1 - c], rc.at[e], a_s.at[e], a_r.at[e], core_id) for e in range(2)
    ]
    for copy in a_copies:
        copy.wait_recv()
    xs[...] = (
        pbuf[2 * (1 - x) + c].astype(f32) + rc[1 - x].astype(f32)
    ).astype(bf16)
    ax = send(xs, rx, a_s.at[2], a_r.at[2], x_id)
    local[1].wait()
    ax.wait_recv()
    total = pbuf[t].astype(f32) + rc[x].astype(f32) + rx[...].astype(f32)
    total = total + res[...].astype(f32)
    mixed[...] = total
    ng[s, t] = (
        total * lax.rsqrt(jnp.mean(total * total, axis=-1, keepdims=True) + norm_eps)
        * mg_ref[...]
    ).astype(bf16)

    own = ng.at[s, t]
    z_copies = [None] + [
        send(own, own, z_s.at[d], z_r.at[d], {"sp": sp_of(d)}) for d in range(1, n)
    ]
    x_copies, c_copies = [], []

    def relay(d):
        piece = ng.at[sp_of(n - d), t]
        x_copies.append(send(piece, piece, x_s.at[d], x_r.at[d], x_id))
        c_copies.append(send(piece, piece, c_s.at[0, d], c_r.at[0, d], core_id))

    relay(0)
    d_copies = []
    y_copies = []
    k = 0
    for d in range(1, n):
        for i, dst in enumerate((wg, wu)):
            w_copies[k].wait_recv()
            k += 1
            piece = dst.at[wrows(sp_of(n - d))]
            y_copies.append(send(piece, piece, y_s.at[i, d], y_r.at[i, d], y_id))

    gate[0:8] = jnp.zeros((8, width), f32)
    gate[n * rows + 8 : n * rows + 16] = jnp.zeros((8, width), f32)
    forwards = []

    def pass_on(d):
        x_copies[d].wait_recv()
        piece = ng.at[sp_of(n - d), lax.rem(t + 2, 4)]
        forwards.append(send(piece, piece, c_s.at[1, d], c_r.at[1, d], core_id))

    def take_next(d):
        z_copies[d].wait_recv()
        relay(d)

    def send_down():
        for d in range(1, n):
            j = sp_of(d)
            rows_j = pl.ds(pl.multiple_of(col_start(j) + g * hw, LANES // 2), hw)
            d_copies.append(
                send(dw_hbm.at[rows_j], wd.at[s, dhalf], w_s.at[2, d], w_r.at[2, d], {"sp": j})
            )

    def project(d):
        if d == 0:
            local[2].wait()
            local[3].wait()
            for copy in y_copies:
                copy.wait_recv()
        c_copies[d].wait_recv()
        forwards[d].wait_recv()
        src = sp_of(n - d)
        tokens = ng[src].reshape(rows, dim)
        at = pl.ds(pl.multiple_of(src * rows + 8, 8), rows)
        gate[at] = jnp.dot(tokens, wg[...], preferred_element_type=f32).astype(bf16).astype(f32)
        up[src] = jnp.dot(tokens, wu[...], preferred_element_type=f32).astype(bf16)

    for d in range(1, n):
        take_next(d)
        if d == n - 1:
            send_down()
        pass_on(d - 1)
        if d >= 2:
            project(d - 2)
    if n > 1:
        project(n - 2)
    pass_on(n - 1)
    project(n - 1)

    yd_copies = {}

    def forward_down(d):
        d_copies[d - 1].wait_recv()
        piece = wd.at[sp_of(n - d), dhalf]
        yd_copies[d] = send(piece, piece, y_s.at[2, d], y_r.at[2, d], y_id)

    forward_down(1)
    column = mine + lax.broadcasted_iota(jnp.int32, (rows, width), 1)
    keep = column >= s * width
    local[5].wait()
    taps = taps_ref[...]
    for r in range(n):
        window = gate[r * rows : (r + 1) * rows + 16]
        conv = (
            taps[0:1] * window[7 : 7 + rows]
            + taps[1:2] * window[8 : 8 + rows]
            + taps[2:3] * window[9 : 9 + rows]
        )
        act = jax.nn.silu(conv) * up[r].astype(f32)
        hid[r * rows : (r + 1) * rows] = jnp.where(keep, act, 0.0).astype(bf16)

    pcs, pxc, pzc = {}, {}, {}

    def stage_a(i):
        if i == 0:
            local[4].wait()
        else:
            yd_copies[i].wait_recv()
        ps[i] = (
            jnp.dot(hid[...], wd[sp_of(n - i)], preferred_element_type=f32).astype(bf16)
            .reshape(n, 4, part, cols)
        )
        pcs[i] = [
            send(ps.at[i, :, 2 * e + 1 - c], prc.at[i, e], pc_s.at[i, e], pc_r.at[i, e], core_id)
            for e in range(2)
        ]

    def stage_b(i):
        for copy in pcs[i]:
            copy.wait_recv()
        pxs[i] = (
            ps[i, :, 2 * (1 - x) + c].astype(f32) + prc[i, 1 - x].astype(f32)
        ).astype(bf16)
        pxc[i] = send(pxs.at[i], prx.at[i], px_s.at[i], px_r.at[i], x_id)

    def columns_of(owner):
        return pl.ds(pl.multiple_of(owner * cols, LANES), cols)

    def stage_c(i):
        pxc[i].wait_recv()
        pzs[i] = (
            ps[i, :, t].astype(f32) + prc[i, x].astype(f32) + prx[i].astype(f32)
        ).astype(bf16)
        for d in range(1, n):
            j = sp_of(d)
            pzc[i, d] = send(
                pzs.at[i, j], pzr.at[i, d], pz_s.at[i, d], pz_r.at[i, d], {"sp": j}
            )
        mixed[:, columns_of(sp_of(n - i))] += (
            ps[i, s, t].astype(f32) + prc[i, x, s].astype(f32) + prx[i, s].astype(f32)
        )

    for i in range(n + 2):
        if i < n:
            stage_a(i)
        if 0 <= i - 1 < n:
            stage_b(i - 1)
        if i + 2 < n:
            forward_down(i + 2)
        if 0 <= i - 2 < n:
            stage_c(i - 2)
    for i in range(n):
        for d in range(1, n):
            pzc[i, d].wait_recv()
            mixed[:, columns_of(sp_of(2 * n - d - i))] += pzr[i, d].astype(f32)
    out_ref[...] = mixed[...].astype(bf16)
    for copy in sends:
        copy.wait_send()


def fused(n, width, queries, keys, values, query_gain, key_norm_gain, out_weight, residual,
          mixer_gain, gate_weight, up_weight, conv_taps, down_weight):
    rows, hd = keys.shape
    dim = residual.shape[1]
    cols = down_weight.shape[1]
    part = rows // 4
    bf16, f32 = jnp.bfloat16, jnp.float32
    s = lax.axis_index("sp")
    positions = s * rows + jnp.arange(rows, dtype=jnp.int32)
    cos, sin = angle_tables(positions, hd)
    odd = (jnp.arange(hd) // (hd // 4)) % 2 == 1
    sa = jnp.where(odd, sin, 0.0)
    sb = jnp.where(odd, 0.0, -sin)
    vm = pl.BlockSpec(memory_space=pltpu.VMEM)
    hbm = pl.BlockSpec(memory_space=pl.ANY)
    dma = pltpu.SemaphoreType.DMA
    V = pltpu.VMEM
    scratch = [
        V((n, rows, 2 * hd), bf16), V((rows, queries.shape[1]), bf16),
        V(out_weight.shape, bf16), V((part, dim), bf16), V((4, part, dim), bf16),
        V((2, part, dim), bf16), V((part, dim), bf16), V((part, dim), bf16), V((part, dim), f32),
        V((n, 4, part, dim), bf16), V((dim, width), bf16), V((dim, width), bf16),
        V((n, width, cols), bf16), V((conv_taps.shape[0], width), f32),
        V((n * rows + 16, width), f32), V((n, rows, width), bf16), V((n * rows, width), bf16),
        V((n, n, 4, part, cols), bf16), V((n, 2, n, part, cols), bf16), V((n, n, part, cols), bf16),
        V((n, n, part, cols), bf16), V((n, n, part, cols), bf16), V((n, n, part, cols), bf16),
        dma((6,)), dma((n,)), dma((n,)), dma((3, n)), dma((3, n)), dma((3, n)), dma((3, n)),
        dma((3,)), dma((3,)), dma((n,)), dma((n,)), dma((n,)), dma((n,)), dma((2, n)),
        dma((2, n)), dma((n, 2)), dma((n, 2)), dma((n,)), dma((n,)), dma((n, n)), dma((n, n)),
    ]
    return pl.pallas_call(
        functools.partial(fused_kernel, n, width),
        out_shape=jax.ShapeDtypeStruct((part, dim), bf16),
        in_specs=[vm] * 9 + [hbm] * 6,
        out_specs=vm,
        scratch_shapes=scratch,
        compiler_params=pltpu.CompilerParams(
            collective_id=0, has_side_effects=True, vmem_limit_bytes=60 * 1024 * 1024
        ),
    )(queries, keys, values, query_gain[None], key_norm_gain[None], cos, sa, sb,
      mixer_gain[None], out_weight, residual, gate_weight, up_weight, down_weight, conv_taps)


def block_width(n, hidden_here):
    return -(-hidden_here // (n * LANES)) * LANES


def dispatch(*args):
    queries, keys, gate_weight = args[0], args[1], args[8]
    n = lax.axis_size("sp")
    hidden_here = gate_weight.shape[1]
    width = block_width(n, hidden_here)
    fits = (n - 1) * width < hidden_here and n * keys.shape[0] <= 2048
    if (
        n > 1 and fits and lax.axis_size("tp") == 4 and lax.axis_size("grp") == 2
        and keys.shape[1] == args[3].shape[0] and keys.shape[0] % 64 == 0
        and hidden_here % LANES == 0
    ):
        return fused(n, width, *args)
    return local(*args)


def solution(mesh):
    in_specs = (
        P(("grp", "sp"), "tp"),
        P(("grp", "sp"), "tp"),
        P(("grp", "sp"), "tp"),
        P(),
        P(),
        P("tp", None),
        P(("grp", "sp"), None),
        P(),
        P("sp", "tp"),
        P("sp", "tp"),
        P(None, "tp"),
        P("tp", "sp"),
    )
    out_specs = P(("grp", "sp", "tp"), None)
    return jax.shard_map(dispatch, mesh=mesh, in_specs=in_specs, out_specs=out_specs, check_vma=False)
```
